32 devices in a mesh: ep: 8 (over z, y), tp: 4 (over x, core).
Axes of the slice: x: 2, y: 2, z: 4, core: 2. Of those that a mesh axis runs over, the one named last changes fastest.
Arguments:
- tokens: bfloat16 [1024, 2048], P('ep'), may hold values from -6 to 6
- norm_gain: float32 [2048], replicated, may hold values from 0.1 to 1.9
- routes: int32 [1024, 2], P('ep'), may hold values from 0 to 7, all different within a row; in each aligned block of 128 rows (0 to 127, 128 to 255, ...) at most 48 rows name the same one
- group_prob: float32 [1024], P('ep'), may hold values from 0.2 to 1
- expert_logits: float32 [1024, 2], P('ep'), may hold values from -6 to 6
- gate_weight: bfloat16 [8, 2048, 384], P('ep', None, 'tp'), may hold values from -0.125 to 0.125
- up_weight: bfloat16 [8, 2048, 384], P('ep', None, 'tp'), may hold values from -0.125 to 0.125
- down_matrix: bfloat16 [8, 384, 2048], P('ep', 'tp'), may hold values from -0.3125 to 0.3125
Outputs:
- combined: bfloat16 [1024, 2048], P('ep', 'tp')
The draws below stay inside these ranges and needn't reach their ends.
Inputs may be any that keep to these rules, and one draw needn't show every extreme that they name: `routes`: each row names 2 different experts. Among the 128 tokens of one index of ep at most 48 rows name one expert, and in every draw some expert is named by exactly 48 of them.
All inputs are finite; a program needn't handle non-finite values.
Results may differ from the reference program's by a relative error of at most 0.013.
Values may be sent and summed in bfloat16 or wider, within the bound.
No kernel may reach another device: no remote copies, remote signals or barrier semaphores. Data moves between devices by JAX's collectives and lax.ppermute only.
A program may use at most 64 MiB of HBM per device.

```python
import math
import jax
import jax.numpy as jnp
import numpy as np
from jax import lax

MODEL_DIM = 2048
FF = 384
TOPK = 2
TOK_DEV = 128
EXPERTS = 8
CAP = 48
TOKENS = 1024
N_EP = 8
N_TP = 4


def shard_levels(key, shape, split, least, high):
    level, own = 1.0, jax.random.fold_in(key, 6)
    for axis_at, shards_of in split:
        draws = jnp.exp(jax.random.uniform(jax.random.fold_in(own, axis_at), (shards_of,), jnp.float32, least / len(split), high / len(split)))
        level = level * jnp.repeat(draws, shape[axis_at] // shards_of).reshape([-1 if axis == axis_at else 1 for axis in range(len(shape))])
    return level


def assign_block(stream_key, own, number, rows, number_of, top, limit, lean):
    sequence = jax.random.permutation(stream_key, number_of)
    heavy_load, common = shares(number_of, rows * top, limit, lean, True), shares(number_of, rows * top, limit, lean, False)
    places = jnp.arange(number_of)

    def named(lengths, turn):
        used = int((lengths > 0).sum())
        fixed = max(1, used // 4)
        passed = fixed + (places - fixed + turn * (used - fixed)) % max(1, number_of - fixed)
        return jnp.zeros((number_of,), jnp.int32).at[sequence[jnp.where(places < fixed, places, passed)]].set(jnp.asarray(lengths, jnp.int32))

    lengths = jnp.where(number % 4 == 0, named(heavy_load, number // 4), named(common, number - number // 4 - 1))
    mixed = jax.random.permutation(jax.random.fold_in(own, 3), number_of)
    giver, receiver = mixed[0:number_of // 2 * 2:2], mixed[1:number_of // 2 * 2:2]
    room = jnp.minimum(lengths[giver] - 1, limit - lengths[receiver]) // 2
    room = jnp.where((giver == sequence[0]) | (receiver == sequence[0]) | (lengths[receiver] == 0), 0, jnp.maximum(room, 0))
    passed = jax.random.randint(jax.random.fold_in(own, 4), (number_of // 2,), 0, 1 << 20) % (room + 1)
    lengths = lengths.at[giver].add(-passed).at[receiver].add(passed)
    labels = jnp.searchsorted(jnp.cumsum(lengths), jnp.arange(rows * top), side="right").astype(jnp.int32)
    listing = labels.reshape(top, rows).T
    listing = listing[jax.random.permutation(jax.random.fold_in(own, 1), rows)]
    turn = jax.random.randint(jax.random.fold_in(own, 2), (rows, 1), 0, top)
    return jnp.take_along_axis(listing, (jnp.arange(top)[None, :] + turn) % top, axis=1)


def shares(amount, total, limit, skew, full):
    portions = [(1 << 20) // math.isqrt(standing ** skew) + 1 for standing in range(1, amount + 1)]
    largest = limit if full else min(limit, max(-(-total // amount), total * portions[0] // sum(portions)))
    least = 1 if total - largest >= amount - 1 else 0
    holding, surplus = [largest] + [least] * (amount - 1), total - largest - least * (amount - 1)
    while surplus > 0:
        movable = [i for i in range(1, amount) if holding[i] < largest] or [i for i in range(1, amount) if holding[i] < limit]
        whole, remaining = sum([portions[i] for i in movable]), surplus
        for i in movable:
            extra = min(limit - holding[i], max(1, remaining * portions[i] // whole), surplus)
            holding[i] = holding[i] + extra
            surplus = surplus - extra
    return np.array(holding)


def bell_draw(rng, dims, spread, bound, shards=(), held_as=jnp.bfloat16):
    drawn = spread * jax.random.normal(rng, dims, jnp.float32)
    if shards:
        drawn = drawn * shard_levels(rng, dims, shards, -0.22, 0.18)
    return jnp.clip(drawn, -bound, bound).astype(held_as)


def setup_inputs(seed: int = 0) -> dict:
    key_of = jax.random.split(jax.random.key(seed), 9)
    tokens = bell_draw(key_of[0], (TOKENS, MODEL_DIM), 1.0, 6.0, ((0, 8),))
    norm_gain = jnp.clip(1.0 + 0.18 * jax.random.normal(key_of[1], (MODEL_DIM,), jnp.float32), 0.1, 1.9)
    routes_keys = jax.random.split(jax.random.fold_in(key_of[2], 1), TOKENS // TOK_DEV)
    routes_turns = jax.random.permutation(jax.random.fold_in(key_of[2], 3), TOKENS // TOK_DEV)
    routes = jax.vmap(lambda own, number: assign_block(jax.random.fold_in(key_of[2], 2), own, number, TOK_DEV, EXPERTS, TOPK, CAP, 2))(routes_keys, routes_turns).reshape((TOKENS, TOPK))
    group_prob = jnp.clip(0.2 + 0.8 * jax.random.uniform(key_of[3], (TOKENS,), jnp.float32) ** shard_levels(key_of[3], (TOKENS,), ((0, 8),), -0.2, 0.2), 0.2, 1.0)
    expert_logits = bell_draw(key_of[4], (TOKENS, TOPK), 1.5, 6.0, ((0, 8),), jnp.float32)
    gate_weight = bell_draw(key_of[5], (EXPERTS, MODEL_DIM, FF), MODEL_DIM ** -0.5, 0.125, ((0, 8), (2, 4)))
    up_weight = bell_draw(key_of[6], (EXPERTS, MODEL_DIM, FF), MODEL_DIM ** -0.5, 0.125, ((0, 8), (2, 4)))
    down_matrix = bell_draw(key_of[7], (EXPERTS, FF, MODEL_DIM), FF ** -0.5, 0.3125, ((0, 8), (1, 4)))
    return {"tokens": tokens, "norm_gain": norm_gain, "routes": routes, "group_prob": group_prob, "expert_logits": expert_logits, "gate_weight": gate_weight, "up_weight": up_weight, "down_matrix": down_matrix}


def reference(tokens, norm_gain, routes, group_prob, expert_logits, gate_weight, up_weight, down_matrix):
    values = tokens.astype(jnp.float32)
    normed = (values * lax.rsqrt(lax.optimization_barrier(jnp.mean(values * values, -1, keepdims=True)) + 1e-06) * norm_gain).astype(jnp.bfloat16)
    weights = group_prob[:, None] * jax.nn.softmax(expert_logits.astype(jnp.float32), axis=-1)
    flat_ids = routes.reshape(-1)
    flat_weights = weights.reshape(-1)
    upper_limit = N_EP * CAP
    slice_width = FF // N_TP

    def visit(total, expert_index):
        hits = flat_ids == expert_index
        found = jnp.nonzero(hits, size=upper_limit, fill_value=0)[0].astype(jnp.int32)
        usable = jnp.arange(upper_limit, dtype=jnp.int32) < jnp.sum(hits.astype(jnp.int32))
        owners = (found // TOPK).astype(jnp.int32)
        inputs = normed[owners]
        gate_proj = jnp.dot(inputs, gate_weight[expert_index], preferred_element_type=jnp.float32)
        up_proj = jnp.dot(inputs, up_weight[expert_index], preferred_element_type=jnp.float32)
        hidden_state = (jax.nn.silu(gate_proj) * up_proj).astype(jnp.bfloat16)
        block_list = jnp.einsum('lzn,znx->zlx', hidden_state.reshape(upper_limit, N_TP, slice_width).astype(jnp.float32), down_matrix[expert_index].reshape(N_TP, slice_width, MODEL_DIM).astype(jnp.float32)).astype(jnp.bfloat16)
        expert_out = lax.optimization_barrier(jnp.sum(block_list.astype(jnp.float32), 0)).astype(jnp.bfloat16)
        scale = jnp.where(usable, flat_weights[found], jnp.zeros((), jnp.float32))
        total = total.at[owners].add(expert_out.astype(jnp.float32) * scale[:, None])
        return (total, None)
    total, _ = lax.scan(visit, jnp.zeros((TOKENS, MODEL_DIM), jnp.float32), jnp.arange(EXPERTS, dtype=jnp.int32))
    return total.astype(jnp.bfloat16)
```

```python
import functools

import jax
import jax.numpy as jnp
from jax import lax
from jax.experimental import pallas as pl
from jax.experimental.pallas import tpu as pltpu
from jax.sharding import PartitionSpec as P

F32, BF16, I32 = jnp.float32, jnp.bfloat16, jnp.int32
VM = pl.BlockSpec(memory_space=pltpu.VMEM)
SM = pl.BlockSpec(memory_space=pltpu.SMEM)


def dot(a, b, ca, cb):
    return lax.dot_general(a, b, (((ca,), (cb,)), ((), ())), preferred_element_type=F32)


def slot_tables(routes, experts, capacity):
    top, count = routes.shape
    expert_of = lax.broadcasted_iota(I32, (experts, count), 0)
    named = routes[0:1] == expert_of
    for k in range(1, top):
        named = named | (routes[k : k + 1] == expert_of)
    ahead = lax.broadcasted_iota(I32, (count, count), 0) < lax.broadcasted_iota(
        I32, (count, count), 1
    )
    ones = jnp.where(named, 1.0, 0.0).astype(BF16)
    earlier = dot(ones, jnp.where(ahead, 1.0, 0.0).astype(BF16), 1, 0)
    place = jnp.where(named, earlier, -1.0).astype(BF16)
    slots = experts * capacity
    inside = lax.broadcasted_iota(I32, (slots, experts), 0) - capacity * lax.broadcasted_iota(
        I32, (slots, experts), 1
    )
    owned = (inside >= 0) & (inside < capacity)
    spread = jnp.where(owned, 1.0, 0.0).astype(BF16)
    own_place = jnp.sum(jnp.where(owned, inside, 0), 1, keepdims=True).astype(F32)
    held = dot(spread, place, 1, 0) == own_place
    return spread, held


def dispatch_kernel(experts, capacity, at_ref, tokens_ref, gain_ref, routes_ref, out_ref):
    width = out_ref.shape[1]
    values = tokens_ref[...].astype(F32)
    scale = lax.rsqrt(jnp.mean(values * values, -1, keepdims=True) + 1e-06)
    here = pl.ds(pl.multiple_of(at_ref[0] * width, width), width)
    normed = (tokens_ref[:, here].astype(F32) * scale * gain_ref[:, here]).astype(BF16)
    _, held = slot_tables(routes_ref[...], experts, capacity)
    picks = jnp.where(held, 1.0, 0.0).astype(BF16)
    out_ref[...] = dot(picks, normed, 1, 0).astype(BF16)


def gates_kernel(experts, capacity, routes_ref, prob_ref, logits_ref, out_ref):
    routes, logits = routes_ref[...], logits_ref[...]
    top, count = routes.shape
    powers = jnp.exp(logits - jnp.max(logits, 0, keepdims=True))
    weights = prob_ref[...] * (powers / jnp.sum(powers, 0, keepdims=True))
    spread, held = slot_tables(routes, experts, capacity)
    expert_of = lax.broadcasted_iota(I32, (experts, count), 0)
    by_expert = jnp.zeros((experts, count), F32)
    for k in range(top):
        by_expert = by_expert + jnp.where(routes[k : k + 1] == expert_of, weights[k : k + 1], 0.0)
    high = by_expert.astype(BF16)
    low = (by_expert - high.astype(F32)).astype(BF16)
    slots = held.shape[0]
    out_ref[0:slots] = jnp.where(held, dot(spread, high, 1, 0), 0.0).astype(BF16)
    out_ref[slots:] = jnp.where(held, dot(spread, low, 1, 0), 0.0).astype(BF16)


def project_kernel(at_ref, mine_ref, other_ref, gate_ref, up_ref, got_ref, full_ref, send_ref):
    width = mine_ref.shape[1]
    here = pl.ds(pl.multiple_of(at_ref[0] * width, width), width)
    there = pl.ds(pl.multiple_of(at_ref[1] * width, width), width)
    near = pl.ds(pl.multiple_of(at_ref[2] * width, width), width)
    far = pl.ds(pl.multiple_of(at_ref[3] * width, width), width)
    first = jnp.concatenate(
        [gate_ref[:, here], up_ref[:, here], got_ref[0, :, near], got_ref[1, :, near]], 0
    )
    second = jnp.concatenate(
        [gate_ref[:, there], up_ref[:, there], got_ref[0, :, far], got_ref[1, :, far]], 0
    )
    total = dot(first, mine_ref[...], 1, 1) + dot(second, other_ref[...], 1, 1)
    full_ref[...] = total
    send_ref[...] = total.astype(BF16)


def hidden_kernel(full_ref, got_ref, out_ref):
    rows = out_ref.shape[0] // 2
    for half in range(2):
        a, b = 2 * rows * half, 2 * rows * (1 - half)
        gate = full_ref[a : a + rows] + got_ref[b : b + rows].astype(F32)
        up = full_ref[a + rows : a + 2 * rows] + got_ref[b + rows : b + 2 * rows].astype(F32)
        out_ref[rows * half : rows * (half + 1)] = (gate / (1.0 + jnp.exp(-gate)) * up).astype(BF16)


def down_kernel(at_ref, mine_ref, other_ref, down_ref, got_ref, pair_ref, out_ref):
    width = out_ref.shape[1]
    here = pl.ds(pl.multiple_of(at_ref[0] * width, width), width)
    near = pl.ds(pl.multiple_of(at_ref[2] * width, width), width)
    hidden = jnp.concatenate([mine_ref[...], other_ref[...]], 0)
    columns = jnp.concatenate([down_ref[:, here], got_ref[2, :, near], pair_ref[...]], 0)
    out_ref[...] = dot(hidden, columns, 0, 0).astype(BF16)


def combine_kernel(gates_ref, back_ref, out_ref):
    slots = back_ref.shape[0]
    back = back_ref[...]
    total = dot(gates_ref[0:slots], back, 0, 0) + dot(gates_ref[slots:], back, 0, 0)
    out_ref[...] = total.astype(BF16)


def call(kernel, shapes, scalars, arrays, name):
    return pl.pallas_call(
        kernel,
        out_shape=shapes,
        in_specs=[SM] * len(scalars) + [VM] * len(arrays),
        out_specs=jax.tree.map(lambda _: VM, shapes),
        name=name,
    )(*scalars, *arrays)


def body(tokens, norm_gain, routes, group_prob, expert_logits, gate_weight, up_weight, down_matrix):
    tok_rows, model_width = tokens.shape
    top = routes.shape[1]
    local, _, block = gate_weight.shape
    ep, tp = lax.axis_size("ep"), lax.axis_size("tp")
    experts = local * ep
    capacity = 3 * top * tok_rows // (2 * experts)
    slots = experts * capacity
    width = model_width // tp
    shape = jax.ShapeDtypeStruct

    q = lax.axis_index("tp").astype(I32)
    at = jnp.stack([q, q ^ 1, q % 2, 1 - q % 2])
    near = [(i, i ^ 1) for i in range(tp)]
    far = [(i, i ^ 2) for i in range(tp)]

    gate, up, down = gate_weight[0].T, up_weight[0].T, down_matrix[0]
    away = (1 - q // 2) * (2 * width)
    packed = jnp.stack(
        [lax.dynamic_slice_in_dim(w, away, 2 * width, 1) for w in (gate, up, down)]
    )
    got = lax.ppermute(packed, "tp", far)

    outgoing = call(
        functools.partial(dispatch_kernel, experts, capacity),
        shape((slots, width), BF16),
        [at],
        [tokens, norm_gain[None], routes.T],
        "dispatch",
    )
    mine = lax.all_to_all(
        outgoing.reshape(ep, slots // ep, width), "ep", split_axis=0, concat_axis=0, tiled=True
    ).reshape(slots, width)
    gates = call(
        functools.partial(gates_kernel, experts, capacity),
        shape((2 * slots, tok_rows), BF16),
        [],
        [routes.T, group_prob[None], expert_logits.T],
        "gates",
    )
    pair = lax.ppermute(
        jnp.concatenate(
            [
                lax.dynamic_slice_in_dim(down, at[1] * width, width, 1),
                lax.dynamic_slice_in_dim(got[2], at[3] * width, width, 1),
            ],
            0,
        ),
        "tp",
        near,
    )
    other = lax.ppermute(mine, "tp", near)
    full, send = call(
        project_kernel,
        (shape((4 * block, slots), F32), shape((4 * block, slots), BF16)),
        [at],
        [mine, other, gate, up, got],
        "project",
    )
    hidden = call(
        hidden_kernel,
        shape((2 * block, slots), BF16),
        [],
        [full, lax.ppermute(send, "tp", far)],
        "hidden",
    )
    summed = call(
        down_kernel,
        shape((slots, width), BF16),
        [at],
        [hidden, lax.ppermute(hidden, "tp", near), down, got, pair],
        "down",
    )
    back = lax.all_to_all(
        summed.reshape(ep, slots // ep, width), "ep", split_axis=0, concat_axis=0, tiled=True
    ).reshape(slots, width)
    return call(combine_kernel, shape((tok_rows, width), BF16), [], [gates, back], "combine")


def solution(mesh):
    return jax.shard_map(
        body,
        mesh=mesh,
        in_specs=(
            P("ep", None),
            P(),
            P("ep", None),
            P("ep"),
            P("ep", None),
            P("ep", None, "tp"),
            P("ep", None, "tp"),
            P("ep", "tp", None),
        ),
        out_specs=P("ep", "tp"),
        check_vma=False,
    )
```

```python
import functools

import jax
import jax.numpy as jnp
from jax import lax
from jax.experimental import pallas as pl
from jax.experimental.pallas import tpu as pltpu
from jax.sharding import PartitionSpec as P


F32, BF16, I32 = jnp.float32, jnp.bfloat16, jnp.int32
VM = pl.BlockSpec(memory_space=pltpu.VMEM)


def dot(a, b, ca, cb):
    return lax.dot_general(a, b, (((ca,), (cb,)), ((), ())), preferred_element_type=F32)


def columns(index, width):
    return pl.ds(pl.multiple_of(index * width, width), width)


def slot_tables(routes, experts, capacity):
    top, count = routes.shape
    expert_of = lax.broadcasted_iota(I32, (experts, count), 0)
    named = routes[0:1] == expert_of
    for k in range(1, top):
        named = named | (routes[k : k + 1] == expert_of)
    ahead = lax.broadcasted_iota(I32, (count, count), 0) < lax.broadcasted_iota(
        I32, (count, count), 1
    )
    ones = jnp.where(named, 1.0, 0.0).astype(BF16)
    earlier = dot(ones, jnp.where(ahead, 1.0, 0.0).astype(BF16), 1, 0)
    place = jnp.where(named, earlier, -1.0).astype(BF16)
    slots = experts * capacity
    inside = lax.broadcasted_iota(I32, (slots, experts), 0) - capacity * lax.broadcasted_iota(
        I32, (slots, experts), 1
    )
    owned = (inside >= 0) & (inside < capacity)
    spread = jnp.where(owned, 1.0, 0.0).astype(BF16)
    own_place = jnp.sum(jnp.where(owned, inside, 0), 1, keepdims=True).astype(F32)
    held = dot(spread, place, 1, 0) == own_place
    return spread, held


def dispatch_kernel(experts, capacity, tokens_ref, gain_ref, routes_ref, out_ref):
    width = out_ref.shape[1]
    values = tokens_ref[...].astype(F32)
    scale = lax.rsqrt(jnp.mean(values * values, -1, keepdims=True) + 1e-06)
    here = columns(lax.axis_index("tp"), width)
    normed = (tokens_ref[:, here].astype(F32) * scale * gain_ref[:, here]).astype(BF16)
    _, held = slot_tables(routes_ref[...], experts, capacity)
    picks = jnp.where(held, 1.0, 0.0).astype(BF16)
    out_ref[...] = dot(picks, normed, 1, 0).astype(BF16)


def gates_kernel(experts, capacity, routes_ref, prob_ref, logits_ref, out_ref):
    routes, logits = routes_ref[...], logits_ref[...]
    top, count = routes.shape
    powers = jnp.exp(logits - jnp.max(logits, 0, keepdims=True))
    weights = prob_ref[...] * (powers / jnp.sum(powers, 0, keepdims=True))
    spread, held = slot_tables(routes, experts, capacity)
    expert_of = lax.broadcasted_iota(I32, (experts, count), 0)
    by_expert = jnp.zeros((experts, count), F32)
    for k in range(top):
        by_expert = by_expert + jnp.where(routes[k : k + 1] == expert_of, weights[k : k + 1], 0.0)
    high = by_expert.astype(BF16)
    low = (by_expert - high.astype(F32)).astype(BF16)
    slots = held.shape[0]
    out_ref[0:slots] = jnp.where(held, dot(spread, high, 1, 0), 0.0).astype(BF16)
    out_ref[slots:] = jnp.where(held, dot(spread, low, 1, 0), 0.0).astype(BF16)


def project_kernel(mine_ref, other_ref, gate_ref, up_ref, got_ref, full_ref, send_ref):
    width = mine_ref.shape[1]
    q = lax.axis_index("tp")
    here, there = columns(q, width), columns(q ^ 1, width)
    near, far = columns(q & 1, width), columns(1 - (q & 1), width)
    first = jnp.concatenate(
        [gate_ref[:, here], up_ref[:, here], got_ref[0, :, near], got_ref[1, :, near]], 0
    )
    second = jnp.concatenate(
        [gate_ref[:, there], up_ref[:, there], got_ref[0, :, far], got_ref[1, :, far]], 0
    )
    total = dot(first, mine_ref[...], 1, 1) + dot(second, other_ref[...], 1, 1)
    full_ref[...] = total
    send_ref[...] = total.astype(BF16)


def hidden_kernel(full_ref, got_ref, out_ref):
    rows = out_ref.shape[0] // 2
    for half in range(2):
        a, b = 2 * rows * half, 2 * rows * (1 - half)
        gate = full_ref[a : a + rows] + got_ref[b : b + rows].astype(F32)
        up = full_ref[a + rows : a + 2 * rows] + got_ref[b + rows : b + 2 * rows].astype(F32)
        out_ref[rows * half : rows * (half + 1)] = (gate / (1.0 + jnp.exp(-gate)) * up).astype(BF16)


def down_kernel(mine_ref, other_ref, down_ref, got_ref, pair_ref, out_ref):
    width = out_ref.shape[1]
    q = lax.axis_index("tp")
    here, near = columns(q, width), columns(q & 1, width)
    hidden = jnp.concatenate([mine_ref[...], other_ref[...]], 0)
    weights = jnp.concatenate([down_ref[:, here], got_ref[2, :, near], pair_ref[...]], 0)
    out_ref[...] = dot(hidden, weights, 0, 0).astype(BF16)


def combine_kernel(gates_ref, back_ref, out_ref):
    slots = back_ref.shape[0]
    back = back_ref[...]
    total = dot(gates_ref[0:slots], back, 0, 0) + dot(gates_ref[slots:], back, 0, 0)
    out_ref[...] = total.astype(BF16)


def call(kernel, shapes, arrays):
    return pl.pallas_call(
        kernel,
        out_shape=shapes,
        in_specs=[VM] * len(arrays),
        out_specs=jax.tree.map(lambda _: VM, shapes),
        compiler_params=pltpu.CompilerParams(vmem_limit_bytes=16 * 2**20),
    )(*arrays)


def body(tokens, norm_gain, routes, group_prob, expert_logits, gate_weight, up_weight, down_matrix):
    tok_rows, model_width = tokens.shape
    top = routes.shape[1]
    local, _, block = gate_weight.shape
    ep, tp = lax.axis_size("ep"), lax.axis_size("tp")
    experts = local * ep
    capacity = 3 * top * tok_rows // (2 * experts)
    slots = experts * capacity
    width = model_width // tp
    shape = jax.ShapeDtypeStruct

    q = lax.axis_index("tp").astype(I32)
    near = [(i, i ^ 1) for i in range(tp)]
    far = [(i, i ^ 2) for i in range(tp)]

    gate, up, down = gate_weight[0].T, up_weight[0].T, down_matrix[0]
    away = (1 - (q >> 1)) * (2 * width)
    packed = jnp.stack(
        [lax.dynamic_slice_in_dim(w, away, 2 * width, 1) for w in (gate, up, down)]
    )
    got = lax.ppermute(packed, "tp", far)

    outgoing = call(
        functools.partial(dispatch_kernel, experts, capacity),
        shape((slots, width), BF16),
        [tokens, norm_gain[None], routes.T],
    )
    mine = lax.all_to_all(
        outgoing.reshape(ep, slots // ep, width), "ep", split_axis=0, concat_axis=0, tiled=True
    ).reshape(slots, width)
    gates = call(
        functools.partial(gates_kernel, experts, capacity),
        shape((2 * slots, tok_rows), BF16),
        [routes.T, group_prob[None], expert_logits.T],
    )
    pair = lax.ppermute(
        jnp.concatenate(
            [
                lax.dynamic_slice_in_dim(down, (q ^ 1) * width, width, 1),
                lax.dynamic_slice_in_dim(got[2], (1 - (q & 1)) * width, width, 1),
            ],
            0,
        ),
        "tp",
        near,
    )
    other = lax.ppermute(mine, "tp", near)
    full, send = call(
        project_kernel,
        (shape((4 * block, slots), F32), shape((4 * block, slots), BF16)),
        [mine, other, gate, up, got],
    )
    hidden = call(
        hidden_kernel, shape((2 * block, slots), BF16), [full, lax.ppermute(send, "tp", far)]
    )
    summed = call(
        down_kernel,
        shape((slots, width), BF16),
        [hidden, lax.ppermute(hidden, "tp", near), down, got, pair],
    )
    back = lax.all_to_all(
        summed.reshape(ep, slots // ep, width), "ep", split_axis=0, concat_axis=0, tiled=True
    ).reshape(slots, width)
    return call(combine_kernel, shape((tok_rows, width), BF16), [gates, back])


def solution(mesh):
    return jax.shard_map(
        body,
        mesh=mesh,
        in_specs=(
            P("ep", None),
            P(),
            P("ep", None),
            P("ep"),
            P("ep", None),
            P("ep", None, "tp"),
            P("ep", None, "tp"),
            P("ep", "tp", None),
        ),
        out_specs=P("ep", "tp"),
        check_vma=False,
    )
```

```python
import functools

import jax
import jax.numpy as jnp
from jax import lax
from jax.experimental import pallas as pl
from jax.experimental.pallas import tpu as pltpu
from jax.sharding import PartitionSpec as P


F32, BF16, I32 = jnp.float32, jnp.bfloat16, jnp.int32
VM = pl.BlockSpec(memory_space=pltpu.VMEM)
HBM = pl.BlockSpec(memory_space=pltpu.HBM)
PARTS = 1


def dot(a, b, ca, cb):
    return lax.dot_general(a, b, (((ca,), (cb,)), ((), ())), preferred_element_type=F32)


def columns(index, width):
    return pl.ds(pl.multiple_of(index * width, width), width)


def chunks(count):
    first = -(-count // 16) * 8
    if PARTS == 1 or first >= count:
        return [(0, count)]
    return [(0, first), (first, count - first)]


def places(routes, experts):
    top, count = routes.shape
    expert_of = lax.broadcasted_iota(I32, (experts, count), 0)
    named = routes[0:1] == expert_of
    for k in range(1, top):
        named = named | (routes[k : k + 1] == expert_of)
    ahead = lax.broadcasted_iota(I32, (count, count), 0) < lax.broadcasted_iota(
        I32, (count, count), 1
    )
    ones = jnp.where(named, 1.0, 0.0).astype(BF16)
    earlier = dot(ones, jnp.where(ahead, 1.0, 0.0).astype(BF16), 1, 0)
    return jnp.where(named, earlier, -1.0).astype(BF16)


def holders(place, base, length):
    experts = place.shape[0]
    rows = experts * length
    inside = lax.broadcasted_iota(I32, (rows, experts), 0) - length * lax.broadcasted_iota(
        I32, (rows, experts), 1
    )
    owned = (inside >= 0) & (inside < length)
    spread = jnp.where(owned, 1.0, 0.0).astype(BF16)
    slot = jnp.sum(jnp.where(owned, inside, 0), 1, keepdims=True) + base
    return spread, dot(spread, place, 1, 0) == slot.astype(F32)


def pack_kernel(gate_ref, up_ref, down_ref, away_ref, away_down_ref, keep_ref, sems):
    width = away_ref.shape[2]
    row = lax.axis_index("tp") >> 1
    here, there = columns(row, width), columns(1 - row, width)
    copies = [
        pltpu.make_async_copy(gate_ref.at[:, there], away_ref.at[0], sems.at[0]),
        pltpu.make_async_copy(up_ref.at[:, there], away_ref.at[1], sems.at[1]),
        pltpu.make_async_copy(down_ref.at[:, there], away_down_ref, sems.at[2]),
        pltpu.make_async_copy(gate_ref.at[:, here], keep_ref.at[0], sems.at[3]),
        pltpu.make_async_copy(up_ref.at[:, here], keep_ref.at[1], sems.at[4]),
        pltpu.make_async_copy(down_ref.at[:, here], keep_ref.at[2], sems.at[5]),
    ]
    for copy in copies:
        copy.start()
    for copy in copies:
        copy.wait()


def dispatch_kernel(experts, half, tokens_ref, gain_ref, routes_ref, *out_refs):
    width = out_refs[0].shape[1]
    q = lax.axis_index("tp")
    values = tokens_ref[...].astype(F32)
    scale = lax.rsqrt(jnp.mean(values * values, -1, keepdims=True) + 1e-06)
    here = columns(q >> 1, width)
    normed = (tokens_ref[:, here].astype(F32) * scale * gain_ref[:, here]).astype(BF16)
    place = places(routes_ref[...], experts)
    for (first, length), out_ref in zip(chunks(half), out_refs):
        _, held = holders(place, (q & 1) * half + first, length)
        out_ref[...] = dot(jnp.where(held, 1.0, 0.0).astype(BF16), normed, 1, 0).astype(BF16)


def gates_kernel(experts, half, routes_ref, prob_ref, logits_ref, *out_refs):
    routes, logits = routes_ref[...], logits_ref[...]
    top, count = routes.shape
    powers = jnp.exp(logits - jnp.max(logits, 0, keepdims=True))
    weights = prob_ref[...] * (powers / jnp.sum(powers, 0, keepdims=True))
    place = places(routes, experts)
    expert_of = lax.broadcasted_iota(I32, (experts, count), 0)
    by_expert = jnp.zeros((experts, count), F32)
    for k in range(top):
        by_expert = by_expert + jnp.where(routes[k : k + 1] == expert_of, weights[k : k + 1], 0.0)
    high = by_expert.astype(BF16)
    low = (by_expert - high.astype(F32)).astype(BF16)
    for (first, length), out_ref in zip(chunks(half), out_refs):
        spread, held = holders(place, (lax.axis_index("tp") & 1) * half + first, length)
        rows = experts * length
        out_ref[0:rows] = jnp.where(held, dot(spread, high, 1, 0), 0.0).astype(BF16)
        out_ref[rows:] = jnp.where(held, dot(spread, low, 1, 0), 0.0).astype(BF16)


def ordered(row, own, far):
    return [jnp.where(row == 0, own, far), jnp.where(row == 0, far, own)]


def project_kernel(mine_ref, keep_ref, far_ref, near_ref, near_far_ref, full_ref, send_ref):
    row = lax.axis_index("tp") >> 1
    pieces = []
    for i in range(2):
        pieces += ordered(row, keep_ref[i], far_ref[i])
        pieces += ordered(row, near_ref[i], near_far_ref[i])
    total = dot(mine_ref[...], jnp.concatenate(pieces, 0), 1, 1)
    full_ref[...] = total
    send_ref[...] = total.astype(BF16)


def expert_kernel(full_ref, got_ref, keep_ref, far_ref, near_ref, near_far_ref, out_ref):
    row = lax.axis_index("tp") >> 1
    width = full_ref.shape[1] // 2
    gate = full_ref[:, :width] + got_ref[:, :width].astype(F32)
    up = full_ref[:, width:] + got_ref[:, width:].astype(F32)
    hidden = (gate / (1.0 + jnp.exp(-gate)) * up).astype(BF16)
    down = ordered(row, keep_ref[2], far_ref[...]) + ordered(row, near_ref[2], near_far_ref[...])
    out_ref[...] = dot(hidden, jnp.concatenate(down, 0), 1, 0).astype(BF16)


def combine_kernel(parts, *refs):
    gates, backs, (own_ref, send_ref) = refs[:parts], refs[parts : 2 * parts], refs[2 * parts :]
    width = own_ref.shape[1]
    column = lax.axis_index("tp") & 1

    def total(at):
        result = None
        for gate_ref, back_ref in zip(gates, backs):
            rows = back_ref.shape[0]
            back = back_ref[:, at]
            part = dot(gate_ref[0:rows], back, 0, 0) + dot(gate_ref[rows:], back, 0, 0)
            result = part if result is None else result + part
        return result

    send_ref[...] = total(columns(1 - column, width)).astype(BF16)
    own_ref[...] = total(columns(column, width))


def call(kernel, shapes, arrays, specs=None, scratch=()):
    return pl.pallas_call(
        kernel,
        out_shape=shapes,
        in_specs=[VM] * len(arrays) if specs is None else specs,
        out_specs=jax.tree.map(lambda _: VM, shapes),
        scratch_shapes=scratch,
        compiler_params=pltpu.CompilerParams(vmem_limit_bytes=16 * 2**20),
    )(*arrays)


def body(tokens, norm_gain, routes, group_prob, expert_logits, gate_weight, up_weight, down_matrix):
    tok_rows, model_width = tokens.shape
    top = routes.shape[1]
    local, _, block = gate_weight.shape
    ep, tp = lax.axis_size("ep"), lax.axis_size("tp")
    experts = local * ep
    capacity = 3 * top * tok_rows // (2 * experts)
    half = -(-capacity // 2)
    width = model_width // 2
    parts = chunks(half)

    def shape(*dims, dtype=BF16):
        return jax.ShapeDtypeStruct(dims, dtype)

    near = [(i, i ^ 1) for i in range(tp)]
    far = [(i, i ^ 2) for i in range(tp)]

    def exchange(x, length):
        blocks = x.reshape(ep, local * length, width)
        return lax.all_to_all(blocks, "ep", split_axis=0, concat_axis=0, tiled=True).reshape(
            x.shape
        )

    away, away_down, keep = call(
        pack_kernel,
        (shape(2, block, width), shape(block, width), shape(3, block, width)),
        [gate_weight[0].T, up_weight[0].T, down_matrix[0]],
        [HBM] * 3,
        [pltpu.SemaphoreType.DMA((6,))],
    )
    got = lax.ppermute(away, "tp", far)
    got_down = lax.ppermute(away_down, "tp", far)
    near_keep = lax.ppermute(keep, "tp", near)
    near_got = lax.ppermute(got, "tp", near)
    near_got_down = lax.ppermute(got_down, "tp", near)

    outgoing = call(
        functools.partial(dispatch_kernel, experts, half),
        tuple(shape(experts * n, width) for _, n in parts),
        [tokens, norm_gain[None], routes.T],
    )
    gates = call(
        functools.partial(gates_kernel, experts, half),
        tuple(shape(2 * experts * n, tok_rows) for _, n in parts),
        [routes.T, group_prob[None], expert_logits.T],
    )
    arrived, projected, backs = [], [], []
    for i, (_, n) in enumerate(parts):
        arrived.append(exchange(outgoing[i], n))
    for i, (_, n) in enumerate(parts):
        full, send = call(
            project_kernel,
            (shape(experts * n, 8 * block, dtype=F32), shape(experts * n, 8 * block)),
            [arrived[i], keep, got, near_keep, near_got],
        )
        projected.append((full, lax.ppermute(send, "tp", far)))
    for i, (_, n) in enumerate(parts):
        summed = call(
            expert_kernel,
            shape(experts * n, width),
            [*projected[i], keep, got_down, near_keep, near_got_down],
        )
        backs.append(exchange(summed, n))
    own, send = call(
        functools.partial(combine_kernel, len(parts)),
        (shape(tok_rows, width // 2, dtype=F32), shape(tok_rows, width // 2)),
        [*gates, *backs],
    )
    return (own + lax.ppermute(send, "tp", near).astype(F32)).astype(BF16)


def solution(mesh):
    return jax.shard_map(
        body,
        mesh=mesh,
        in_specs=(
            P("ep", None),
            P(),
            P("ep", None),
            P("ep"),
            P("ep", None),
            P("ep", None, "tp"),
            P("ep", None, "tp"),
            P("ep", "tp", None),
        ),
        out_specs=P("ep", "tp"),
        check_vma=False,
    )
```

```python
import functools

import jax
import jax.numpy as jnp
from jax import lax
from jax.experimental import pallas as pl
from jax.experimental.pallas import tpu as pltpu
from jax.sharding import PartitionSpec as P


F32, BF16, I32 = jnp.float32, jnp.bfloat16, jnp.int32
VM = pl.BlockSpec(memory_space=pltpu.VMEM)
HBM = pl.BlockSpec(memory_space=pltpu.HBM)


def dot(a, b, ca=1, cb=0):
    return lax.dot_general(a, b, (((ca,), (cb,)), ((), ())), preferred_element_type=F32)


def columns(index, width):
    return pl.ds(pl.multiple_of(index * width, width), width)


def iota(shape, axis):
    return lax.broadcasted_iota(I32, shape, axis)


def split(index, size):
    whole = ((index.astype(F32) + 0.5) * (1.0 / size)).astype(I32)
    return whole, index - size * whole


def mark(condition):
    return jnp.where(condition, 1.0, 0.0).astype(BF16)


def places(routes, experts):
    top, count = routes.shape
    expert_of = iota((experts, count), 0)
    named = routes[0:1] == expert_of
    for k in range(1, top):
        named = named | (routes[k : k + 1] == expert_of)
    ahead = iota((count, count), 0) < iota((count, count), 1)
    return jnp.where(named, dot(mark(named), mark(ahead)), -1.0).astype(BF16)


def pack_kernel(gate_hbm, up_hbm, tokens_hbm, gain_hbm, routes_hbm, *refs):
    away_ref, keep_ref, tokens_ref, gain_ref, routes_ref, sems = refs
    width = away_ref.shape[2]
    row = lax.axis_index("tp") >> 1
    here, there = columns(row, width), columns(1 - row, width)
    pairs = [
        (gate_hbm.at[:, there], away_ref.at[0]),
        (up_hbm.at[:, there], away_ref.at[1]),
        (tokens_hbm, tokens_ref),
        (gain_hbm, gain_ref),
        (routes_hbm, routes_ref),
        (gate_hbm.at[:, here], keep_ref.at[0]),
        (up_hbm.at[:, here], keep_ref.at[1]),
    ]
    copies = [pltpu.make_async_copy(a, b, sems.at[i]) for i, (a, b) in enumerate(pairs)]
    for copy in copies:
        copy.start()
    for copy in copies:
        copy.wait()


def dispatch_kernel(experts, half, tokens_ref, gain_ref, routes_ref, out_ref):
    width = out_ref.shape[1]
    q = lax.axis_index("tp")
    here = columns(q >> 1, width)
    values = tokens_ref[...].astype(F32)
    scale = lax.rsqrt(jnp.mean(values * values, -1, keepdims=True) + 1e-06)
    normed = (tokens_ref[:, here].astype(F32) * scale * gain_ref[:, here]).astype(BF16)
    rows = experts * half
    owner, _ = split(iota((rows, experts), 0), half)
    _, slot = split(iota((rows, 1), 0), half)
    place = places(routes_ref[...], experts)
    spread = mark(owner == iota((rows, experts), 1))
    held = dot(spread, place) == (slot + (q & 1) * half).astype(F32)
    out_ref[...] = dot(mark(held), normed).astype(BF16)


def gates_kernel(experts, quarter, ranks, routes_ref, prob_ref, logits_ref, out_ref):
    routes, logits = routes_ref[...], logits_ref[...]
    top, count = routes.shape
    powers = jnp.exp(logits - jnp.max(logits, 0, keepdims=True))
    weights = prob_ref[...] * (powers / jnp.sum(powers, 0, keepdims=True))
    expert_of = iota((experts, count), 0)
    by_expert = jnp.zeros((experts, count), F32)
    for k in range(top):
        by_expert = by_expert + jnp.where(routes[k : k + 1] == expert_of, weights[k : k + 1], 0.0)
    high = by_expert.astype(BF16)
    low = (by_expert - high.astype(F32)).astype(BF16)
    rows = experts * ranks * 2 * quarter
    owner, _ = split(iota((rows, experts), 0), ranks * 2 * quarter)
    _, inside = split(iota((rows, 1), 0), ranks * 2 * quarter)
    rank, inside = split(inside, 2 * quarter)
    _, slot = split(inside, quarter)
    slot = slot + ((rank & 1) * 2 + (rank >> 1)) * quarter
    spread = mark(owner == iota((rows, experts), 1))
    held = dot(spread, places(routes, experts)) == slot.astype(F32)
    for i, value in enumerate((high, low)):
        out_ref[i] = jnp.where(held, dot(spread, value), 0.0).T.astype(BF16)


def ordered(row, own, far):
    return [jnp.where(row == 0, own, far), jnp.where(row == 0, far, own)]


def project_kernel(quarter, mine_ref, keep_ref, far_ref, near_ref, near_far_ref, *out_refs):
    full_ref, send_ref = out_refs
    row = lax.axis_index("tp") >> 1
    rows = full_ref.shape[0]
    source, slot = split(iota((rows, 1), 0), quarter)
    at = source * 2 * quarter + slot
    slots = iota((rows, 2 * rows), 1)
    picks = jnp.concatenate(
        [mark(slots == at + row * quarter), mark(slots == at + (1 - row) * quarter)], 0
    )
    pieces = []
    for i in range(2):
        pieces += ordered(row, keep_ref[i], far_ref[i])
        pieces += ordered(row, near_ref[i], near_far_ref[i])
    picked = dot(picks, mine_ref[...]).astype(BF16)
    total = dot(picked, jnp.concatenate(pieces, 0), 1, 1)
    full_ref[...] = total[:rows]
    send_ref[...] = total[rows:].astype(BF16)


def expert_kernel(quarter, full_ref, got_ref, down_ref, far_ref, near_ref, near_far_ref, out_ref):
    row = lax.axis_index("tp") >> 1
    sources, ranks, _, width = out_ref.shape
    count = full_ref.shape[0]
    units = full_ref.shape[1] // 2
    gate = full_ref[:, :units] + got_ref[:, :units].astype(F32)
    up = full_ref[:, units:] + got_ref[:, units:].astype(F32)
    hidden = (gate / (1.0 + jnp.exp(-gate)) * up).astype(BF16)
    source, inside = split(iota((2 * count, 1), 0), 2 * quarter)
    part, slot = split(inside, quarter)
    twice = dot(mark(iota((2 * count, count), 1) == source * quarter + slot), hidden).astype(BF16)
    down = jnp.concatenate(
        ordered(row, down_ref[...], far_ref[...]) + ordered(row, near_ref[...], near_far_ref[...]),
        0,
    )
    for rank in range(ranks):
        first = 2 * rank * width
        both = dot(twice, down[:, first : first + 2 * width])
        chosen = jnp.where(part == 0, both[:, :width], both[:, width:])
        out_ref[:, rank] = chosen.reshape(sources, 2 * quarter, width).astype(BF16)


def combine_kernel(quarter, gates_ref, back_ref, out_ref):
    back = back_ref[...]
    width = back.shape[1]
    _, inside = split(iota((1, back.shape[0]), 1), 2 * quarter)
    for f in range(2):
        part = mark((inside >= quarter) == (f == 1))
        total = dot(gates_ref[0] * part, back) + dot(gates_ref[1] * part, back)
        out_ref[:, f * width : (f + 1) * width] = total.astype(BF16)


def call(kernel, shapes, arrays, specs=None, scratch=()):
    return pl.pallas_call(
        kernel,
        out_shape=shapes,
        in_specs=[VM] * len(arrays) if specs is None else specs,
        out_specs=jax.tree.map(lambda _: VM, shapes),
        scratch_shapes=scratch,
        compiler_params=pltpu.CompilerParams(vmem_limit_bytes=16 * 2**20),
    )(*arrays)


def body(tokens, norm_gain, routes, group_prob, expert_logits, gate_weight, up_weight, down_matrix):
    tok_rows, model_width = tokens.shape
    top = routes.shape[1]
    local, _, block = gate_weight.shape
    ep, tp = lax.axis_size("ep"), lax.axis_size("tp")
    experts = local * ep
    capacity = 3 * top * tok_rows // (2 * experts)
    quarter = -(-capacity // 4)
    half = 2 * quarter
    width = model_width // 2
    out_width = model_width // tp

    def shape(*dims, dtype=BF16):
        return jax.ShapeDtypeStruct(dims, dtype)

    near = [(i, i ^ 1) for i in range(tp)]
    far = [(i, i ^ 2) for i in range(tp)]

    down = down_matrix[0]
    held = [gate_weight[0].T, up_weight[0].T, tokens, norm_gain[None], routes.T]
    away, keep, *token_arrays = call(
        pack_kernel,
        (
            shape(2, block, width),
            shape(2, block, width),
            shape(*tokens.shape),
            shape(1, model_width, dtype=F32),
            shape(top, tok_rows, dtype=I32),
        ),
        [pltpu.with_memory_space_constraint(x, pltpu.HBM) for x in held],
        [HBM] * len(held),
        [pltpu.SemaphoreType.DMA((7,))],
    )
    got = lax.ppermute(away, "tp", far)
    got_down = lax.ppermute(down, "tp", far)
    near_keep = lax.ppermute(keep, "tp", near)
    near_down = lax.ppermute(down, "tp", near)
    near_got = lax.ppermute(got, "tp", near)
    near_got_down = lax.ppermute(got_down, "tp", near)

    outgoing = call(
        functools.partial(dispatch_kernel, experts, half),
        shape(experts * half, width),
        token_arrays,
    )
    gates = call(
        functools.partial(gates_kernel, experts, quarter, tp),
        shape(2, tok_rows, experts * tp * half),
        [token_arrays[2], group_prob[None], expert_logits.T],
    )
    mine = lax.all_to_all(
        outgoing.reshape(ep, half, width), "ep", split_axis=0, concat_axis=0, tiled=True
    ).reshape(ep * half, width)
    mine, gates = lax.optimization_barrier((mine, gates))
    full, send = call(
        functools.partial(project_kernel, quarter),
        (shape(ep * quarter, 2 * tp * block, dtype=F32), shape(ep * quarter, 2 * tp * block)),
        [mine, keep, got, near_keep, near_got],
    )
    partial = lax.ppermute(send, "tp", far)
    summed = call(
        functools.partial(expert_kernel, quarter),
        shape(ep, tp, half, out_width // 2),
        [full, partial, down, got_down, near_down, near_got_down],
    )
    back = lax.all_to_all(
        summed.reshape(ep * tp, half, out_width // 2),
        ("ep", "tp"),
        split_axis=0,
        concat_axis=0,
        tiled=True,
    ).reshape(ep * tp * half, out_width // 2)
    return call(
        functools.partial(combine_kernel, quarter), shape(tok_rows, out_width), [gates, back]
    )


def solution(mesh):
    return jax.shard_map(
        body,
        mesh=mesh,
        in_specs=(
            P("ep", None),
            P(),
            P("ep", None),
            P("ep"),
            P("ep", None),
            P("ep", None, "tp"),
            P("ep", None, "tp"),
            P("ep", "tp", None),
        ),
        out_specs=P("ep", "tp"),
        check_vma=False,
    )
```

```python
import functools

import jax
import jax.numpy as jnp
from jax import lax
from jax.experimental import pallas as pl
from jax.experimental.pallas import tpu as pltpu
from jax.sharding import PartitionSpec as P


F32, BF16, I32 = jnp.float32, jnp.bfloat16, jnp.int32
VM = pl.BlockSpec(memory_space=pltpu.VMEM)
HBM = pl.BlockSpec(memory_space=pltpu.HBM)


def dot(a, b, ca=1, cb=0):
    return lax.dot_general(a, b, (((ca,), (cb,)), ((), ())), preferred_element_type=F32)


def columns(index, width):
    return pl.ds(pl.multiple_of(index * width, width), width)


def iota(shape, axis):
    return lax.broadcasted_iota(I32, shape, axis)


def split(index, size):
    whole = ((index.astype(F32) + 0.5) * (1.0 / size)).astype(I32)
    return whole, index - size * whole


def mark(condition):
    return jnp.where(condition, 1.0, 0.0).astype(BF16)


def places(routes, experts):
    top, count = routes.shape
    expert_of = iota((experts, count), 0)
    named = routes[0:1] == expert_of
    for k in range(1, top):
        named = named | (routes[k : k + 1] == expert_of)
    ahead = iota((count, count), 0) < iota((count, count), 1)
    return jnp.where(named, dot(mark(named), mark(ahead)), -1.0).astype(BF16)


def front_kernel(
    experts, half, tokens_hbm, gain_hbm, routes_hbm, gate_hbm, up_hbm, *refs
):
    out_ref, away_ref, keep_ref, tokens_ref, gain_ref, routes_ref, sems = refs
    width = out_ref.shape[1]
    q = lax.axis_index("tp")
    row = q >> 1
    here, there = columns(row, width), columns(1 - row, width)
    pairs = [
        (tokens_hbm, tokens_ref),
        (gain_hbm, gain_ref),
        (routes_hbm, routes_ref),
        (gate_hbm.at[:, there], away_ref.at[0]),
        (up_hbm.at[:, there], away_ref.at[1]),
        (gate_hbm.at[:, here], keep_ref.at[0]),
        (up_hbm.at[:, here], keep_ref.at[1]),
    ]
    copies = [pltpu.make_async_copy(a, b, sems.at[i]) for i, (a, b) in enumerate(pairs)]
    for copy in copies:
        copy.start()
    rows = experts * half
    owner, _ = split(iota((rows, experts), 0), half)
    _, slot = split(iota((rows, 1), 0), half)
    copies[2].wait()
    place = places(routes_ref[...], experts)
    spread = mark(owner == iota((rows, experts), 1))
    held = mark(dot(spread, place) == (slot + (q & 1) * half).astype(F32))
    copies[0].wait()
    copies[1].wait()
    values = tokens_ref[...].astype(F32)
    scale = lax.rsqrt(jnp.mean(values * values, -1, keepdims=True) + 1e-06)
    normed = (tokens_ref[:, here].astype(F32) * scale * gain_ref[:, here]).astype(BF16)
    out_ref[...] = dot(held, normed).astype(BF16)
    for copy in copies[3:]:
        copy.wait()


def gates_kernel(experts, quarter, ranks, routes_ref, prob_ref, logits_ref, out_ref):
    routes, logits = routes_ref[...], logits_ref[...]
    top, count = routes.shape
    powers = jnp.exp(logits - jnp.max(logits, 0, keepdims=True))
    weights = prob_ref[...] * (powers / jnp.sum(powers, 0, keepdims=True))
    expert_of = iota((experts, count), 0)
    by_expert = jnp.zeros((experts, count), F32)
    for k in range(top):
        by_expert = by_expert + jnp.where(routes[k : k + 1] == expert_of, weights[k : k + 1], 0.0)
    high = by_expert.astype(BF16)
    low = (by_expert - high.astype(F32)).astype(BF16)
    rows = experts * ranks * 2 * quarter
    owner, _ = split(iota((rows, experts), 0), ranks * 2 * quarter)
    _, inside = split(iota((rows, 1), 0), ranks * 2 * quarter)
    rank, inside = split(inside, 2 * quarter)
    _, slot = split(inside, quarter)
    slot = slot + ((rank & 1) * 2 + (rank >> 1)) * quarter
    spread = mark(owner == iota((rows, experts), 1))
    held = dot(spread, places(routes, experts)) == slot.astype(F32)
    for i, value in enumerate((high, low)):
        out_ref[i] = jnp.where(held, dot(spread, value), 0.0).T.astype(BF16)


def ordered(row, own, far):
    return [jnp.where(row == 0, own, far), jnp.where(row == 0, far, own)]


def project_kernel(quarter, mine_ref, keep_ref, far_ref, near_ref, near_far_ref, *out_refs):
    full_ref, send_ref = out_refs
    row = lax.axis_index("tp") >> 1
    rows = full_ref.shape[0]
    source, slot = split(iota((rows, 1), 0), quarter)
    at = source * 2 * quarter + slot
    slots = iota((rows, 2 * rows), 1)
    picks = jnp.concatenate(
        [mark(slots == at + row * quarter), mark(slots == at + (1 - row) * quarter)], 0
    )
    pieces = []
    for i in range(2):
        pieces += ordered(row, keep_ref[i], far_ref[i])
        pieces += ordered(row, near_ref[i], near_far_ref[i])
    picked = dot(picks, mine_ref[...]).astype(BF16)
    total = dot(picked, jnp.concatenate(pieces, 0), 1, 1)
    full_ref[...] = total[:rows]
    send_ref[...] = total[rows:].astype(BF16)


def expert_kernel(quarter, full_ref, got_ref, down_ref, far_ref, near_ref, near_far_ref, out_ref):
    row = lax.axis_index("tp") >> 1
    sources, ranks, _, width = out_ref.shape
    count = full_ref.shape[0]
    units = full_ref.shape[1] // 2
    gate = full_ref[:, :units] + got_ref[:, :units].astype(F32)
    up = full_ref[:, units:] + got_ref[:, units:].astype(F32)
    hidden = (gate / (1.0 + jnp.exp(-gate)) * up).astype(BF16)
    source, inside = split(iota((2 * count, 1), 0), 2 * quarter)
    part, slot = split(inside, quarter)
    twice = dot(mark(iota((2 * count, count), 1) == source * quarter + slot), hidden).astype(BF16)
    down = jnp.concatenate(
        ordered(row, down_ref[...], far_ref[...]) + ordered(row, near_ref[...], near_far_ref[...]),
        0,
    )
    for rank in range(ranks):
        first = 2 * rank * width
        both = dot(twice, down[:, first : first + 2 * width])
        chosen = jnp.where(part == 0, both[:, :width], both[:, width:])
        out_ref[:, rank] = chosen.reshape(sources, 2 * quarter, width).astype(BF16)


def combine_kernel(quarter, gates_ref, back_ref, out_ref):
    back = back_ref[...]
    width = back.shape[1]
    _, inside = split(iota((1, back.shape[0]), 1), 2 * quarter)
    for f in range(2):
        part = mark((inside >= quarter) == (f == 1))
        total = dot(gates_ref[0] * part, back) + dot(gates_ref[1] * part, back)
        out_ref[:, f * width : (f + 1) * width] = total.astype(BF16)


def call(kernel, shapes, arrays, specs=None, scratch=()):
    return pl.pallas_call(
        kernel,
        out_shape=shapes,
        in_specs=[VM] * len(arrays) if specs is None else specs,
        out_specs=jax.tree.map(lambda _: VM, shapes),
        scratch_shapes=scratch,
        compiler_params=pltpu.CompilerParams(vmem_limit_bytes=16 * 2**20),
    )(*arrays)


def body(tokens, norm_gain, routes, group_prob, expert_logits, gate_weight, up_weight, down_matrix):
    tok_rows, model_width = tokens.shape
    top = routes.shape[1]
    local, _, block = gate_weight.shape
    ep, tp = lax.axis_size("ep"), lax.axis_size("tp")
    experts = local * ep
    capacity = 3 * top * tok_rows // (2 * experts)
    quarter = -(-capacity // 4)
    half = 2 * quarter
    width = model_width // 2
    out_width = model_width // tp

    def shape(*dims, dtype=BF16):
        return jax.ShapeDtypeStruct(dims, dtype)

    near = [(i, i ^ 1) for i in range(tp)]
    far = [(i, i ^ 2) for i in range(tp)]

    down = down_matrix[0]
    inputs = [tokens, norm_gain[None], routes.T, gate_weight[0].T, up_weight[0].T]
    outgoing, away, keep = call(
        functools.partial(front_kernel, experts, half),
        (shape(experts * half, width), shape(2, block, width), shape(2, block, width)),
        [pltpu.with_memory_space_constraint(x, pltpu.HBM) for x in inputs],
        [HBM] * len(inputs),
        [
            pltpu.VMEM(tokens.shape, BF16),
            pltpu.VMEM((1, model_width), F32),
            pltpu.VMEM((top, tok_rows), I32),
            pltpu.SemaphoreType.DMA((7,)),
        ],
    )
    got = lax.ppermute(away, "tp", far)
    got_down = lax.ppermute(down, "tp", far)
    near_keep = lax.ppermute(keep, "tp", near)
    near_down = lax.ppermute(down, "tp", near)
    near_got = lax.ppermute(got, "tp", near)
    near_got_down = lax.ppermute(got_down, "tp", near)

    gates = call(
        functools.partial(gates_kernel, experts, quarter, tp),
        shape(2, tok_rows, experts * tp * half),
        [routes.T, group_prob[None], expert_logits.T],
    )
    mine = lax.all_to_all(
        outgoing.reshape(ep, half, width), "ep", split_axis=0, concat_axis=0, tiled=True
    ).reshape(ep * half, width)
    mine, gates = lax.optimization_barrier((mine, gates))
    full, send = call(
        functools.partial(project_kernel, quarter),
        (shape(ep * quarter, 2 * tp * block, dtype=F32), shape(ep * quarter, 2 * tp * block)),
        [mine, keep, got, near_keep, near_got],
    )
    partial = lax.ppermute(send, "tp", far)
    summed = call(
        functools.partial(expert_kernel, quarter),
        shape(ep, tp, half, out_width // 2),
        [full, partial, down, got_down, near_down, near_got_down],
    )
    back = lax.all_to_all(
        summed.reshape(ep * tp, half, out_width // 2),
        ("ep", "tp"),
        split_axis=0,
        concat_axis=0,
        tiled=True,
    ).reshape(ep * tp * half, out_width // 2)
    return call(
        functools.partial(combine_kernel, quarter), shape(tok_rows, out_width), [gates, back]
    )


def solution(mesh):
    return jax.shard_map(
        body,
        mesh=mesh,
        in_specs=(
            P("ep", None),
            P(),
            P("ep", None),
            P("ep"),
            P("ep", None),
            P("ep", None, "tp"),
            P("ep", None, "tp"),
            P("ep", "tp", None),
        ),
        out_specs=P("ep", "tp"),
        check_vma=False,
    )
```
